32 devices in a mesh: sp: 8 (over z, x), tp: 4 (over y, core).
Axes of the slice: x: 2, y: 2, z: 4, core: 2. Of those that a mesh axis runs over, the one named last changes fastest.
Arguments:
- cotangent: bfloat16 [1024, 2048], P('sp'), may hold values from -6 to 6
- layer_input: bfloat16 [1024, 2048], P('sp'), may hold values from -6 to 6
- group_choice: int32 [1024], P('sp'), may hold values from 0 to 1, as said below
- inner_pair: int32 [1024, 2], P('sp'), may hold values from 0 to 3, as said below
- group_weight: float32 [1024], P('sp'), may hold values from 0.25 to 1
- inner_logits: float32 [1024, 2], P('sp'), may hold values from -6 to 6
- w_gate: bfloat16 [8, 2048, 2048], P('sp', 'tp'), may hold values from -0.125 to 0.125
- w_up: bfloat16 [8, 2048, 2048], P('sp', 'tp'), may hold values from -0.125 to 0.125
- w_down: bfloat16 [8, 2048, 2048], P('sp', 'tp'), may hold values from -0.125 to 0.125
- outer_gate: bfloat16 [2048, 1024], P('tp', 'sp'), may hold values from -6 to 6
- inner_gate: bfloat16 [2048, 1024], P('tp', 'sp'), may hold values from -6 to 6
- value_stream: bfloat16 [2048, 1024], P('tp', 'sp'), may hold values from -6 to 6
- conv_out: bfloat16 [2048, 1024], P('tp', 'sp'), may hold values from -6 to 6
- conv_taps: float32 [3, 2048], P(None, 'tp'), may hold values from -4 to 4
- w_out: bfloat16 [2048, 2048], P(None, 'tp'), may hold values from -0.125 to 0.125
Outputs:
- grad_input: bfloat16 [1024, 2048], P('sp', 'tp')
- grad_w_gate: bfloat16 [8, 2048, 2048], P('sp', 'tp')
- grad_w_up: bfloat16 [8, 2048, 2048], P('sp', 'tp')
- grad_w_down: bfloat16 [8, 2048, 2048], P('sp', 'tp')
- grad_w_out: float32 [2048, 2048], P('sp', 'tp')
- grad_outer_gate: bfloat16 [2048, 1024], P('tp', 'sp')
- grad_inner_gate: bfloat16 [2048, 1024], P('tp', 'sp')
- grad_value_stream: bfloat16 [2048, 1024], P('tp', 'sp')
The draws below stay inside these ranges and needn't reach their ends.
Inputs may be any that keep to these rules, and one draw needn't show every extreme that they name: Within each block of 128 positions of the sp order, every expert 4 * group_choice + inner_pair is named by at most 52 positions; in every block the 4 experts of one group, the same group for all blocks, are each named by exactly 52 positions. `inner_pair`: the two entries of a position differ.
All inputs are finite; a program needn't handle non-finite values.
Results may differ from the reference program's by a relative error of at most 0.019.
Values may be sent and summed in bfloat16 or wider, within the bound.
A program may use at most 64 MiB of HBM per device.

```python
import math
import jax
import jax.numpy as jnp
from jax import lax

D = 2048
FF = 2048
W = 2048
TAPS = 3
INNER = 4
TOK_DEV = 128
TOKENS = 1024
EXPERTS = 8
GROUPS = 2
CAP = 52
HID_BLOCKS = 4


def route_plan(key):
    blocks = TOKENS // TOK_DEV
    group_span = 2 * CAP
    slot_count = GROUPS * group_span
    full_group = jax.random.randint(jax.random.fold_in(key, 7001), (), 0, GROUPS)

    def one_block(block):
        block_key = jax.random.fold_in(key, block)
        ranking = jax.random.permutation(jax.random.fold_in(block_key, 1), slot_count).astype(jnp.int32)
        owning = jnp.arange(slot_count, dtype=jnp.int32) // group_span
        scores = jnp.where(owning == full_group, ranking - slot_count, ranking)
        chosen = jnp.argsort(scores, stable=True)[:TOK_DEV].astype(jnp.int32)
        shuffle = jax.random.permutation(jax.random.fold_in(block_key, 2), TOK_DEV)
        chosen = chosen[shuffle]
        group_ids = chosen // group_span
        within = chosen % group_span
        first_pick = within % 4
        second_pick = (first_pick + 1 + within // 4 % 3) % 4
        rotation = jax.random.randint(jax.random.fold_in(block_key, 3), (GROUPS,), 0, 4)[group_ids]
        picks = jnp.stack([(first_pick + rotation) % 4, (second_pick + rotation) % 4], axis=1)
        return (group_ids.astype(jnp.int32), picks.astype(jnp.int32))
    group_ids, picks = jax.vmap(one_block)(jnp.arange(blocks))
    return (group_ids.reshape(TOKENS), picks.reshape(TOKENS, 2))


def draw_group_choice(key, part):
    return route_plan(key)[0]


def draw_inner_pair(key, part):
    return route_plan(key)[1]


def spiked(values, stream_key, source, target, blocks, factor):
    def block_of(axis_at):
        return (jnp.arange(values.shape[axis_at]) // (values.shape[axis_at] // blocks)).reshape((-1,) + (1,) * (values.ndim - 1 - axis_at))

    near = jax.random.permutation(stream_key, blocks)[block_of(target)]
    other_side = (block_of(target) + blocks // 2) % blocks
    return jnp.where((block_of(source) == near) | (block_of(source) == other_side), factor * values, values)


def block_scale(stream_key, shape, cuts, least, high):
    def one(dim, shards_of):
        draws = jax.random.uniform(jax.random.fold_in(jax.random.fold_in(stream_key, 6), dim), (shards_of,), jnp.float32, least / len(cuts), high / len(cuts))
        return jnp.repeat(jnp.exp(draws), shape[dim] // shards_of).reshape((-1,) + (1,) * (len(shape) - dim - 1))

    loudness = one(*cuts[0])
    for cut in cuts[1:]:
        loudness = loudness * one(*cut)
    return loudness


def centred(own_key, extent, deviation, bound, split=(), kind=jnp.bfloat16):
    array = jax.random.normal(own_key, extent, jnp.float32) * deviation
    if len(split) > 0:
        array = block_scale(own_key, extent, split, -0.22, 0.18) * array
    return jnp.clip(array, min=-bound, max=bound).astype(kind)


def noise_with(rng, dims, deviation, bound, shards, heavy, kind=jnp.bfloat16):
    values = deviation * jax.random.normal(rng, dims, jnp.float32)
    if shards:
        values = values * block_scale(rng, dims, shards, -0.22, 0.18)
    return jnp.clip(spiked(values, jax.random.fold_in(rng, 3), *heavy), -bound, bound).astype(kind)


def setup_inputs(seed: int = 0) -> dict:
    arg_keys = jax.random.split(jax.random.key(seed), 16)
    cotangent = noise_with(arg_keys[0], (TOKENS, D), 1.0, 6.0, ((0, 8),), (0, 1, 8, 2.0))
    layer_input = centred(arg_keys[1], (TOKENS, D), 1.0, 6.0, ((0, 8),))
    group_choice = draw_group_choice(jax.random.fold_in(arg_keys[15], 71), 0)
    inner_pair = draw_inner_pair(jax.random.fold_in(arg_keys[15], 71), 0)
    group_weight = jnp.clip(jnp.exp(math.log(1.0) - 1.3862944 * jax.random.uniform(arg_keys[4], (TOKENS,), jnp.float32) ** block_scale(arg_keys[4], (TOKENS,), ((0, 8),), -0.2, 0.2)), 0.25, 1.0)
    inner_logits = centred(arg_keys[5], (TOKENS, 2), 1.5, 6.0, ((0, 8),), jnp.float32)
    w_gate = centred(arg_keys[6], (EXPERTS, FF, D), D ** -0.5, 0.125, ((0, 8), (1, 4)))
    w_up = centred(arg_keys[7], (EXPERTS, FF, D), D ** -0.5, 0.125, ((0, 8), (1, 4)))
    w_down = centred(arg_keys[8], (EXPERTS, FF, D), FF ** -0.5, 0.125, ((0, 8), (1, 4)))
    outer_gate = centred(arg_keys[9], (W, TOKENS), 1.0, 6.0, ((0, 4), (1, 8)))
    inner_gate = centred(arg_keys[10], (W, TOKENS), 1.0, 6.0, ((0, 4), (1, 8)))
    value_stream = centred(arg_keys[11], (W, TOKENS), 1.0, 6.0, ((0, 4), (1, 8)))
    conv_out = centred(arg_keys[12], (W, TOKENS), 1.0, 6.0, ((0, 4), (1, 8)))
    conv_taps = centred(arg_keys[13], (TAPS, W), 0.6, 4.0, ((1, 4),), jnp.float32)
    w_out = centred(arg_keys[14], (D, W), W ** -0.5, 0.125, ((1, 4),))
    return {"cotangent": cotangent, "layer_input": layer_input, "group_choice": group_choice, "inner_pair": inner_pair, "group_weight": group_weight, "inner_logits": inner_logits, "w_gate": w_gate, "w_up": w_up, "w_down": w_down, "outer_gate": outer_gate, "inner_gate": inner_gate, "value_stream": value_stream, "conv_out": conv_out, "conv_taps": conv_taps, "w_out": w_out}


def slot_table(group_choice, inner_pair):
    expert_ids = (INNER * group_choice[:, None] + inner_pair).astype(jnp.int32)
    blocks = TOKENS // TOK_DEV
    flat_ids = expert_ids.reshape(blocks, TOK_DEV * 2)
    onehot = (flat_ids[:, :, None] == jnp.arange(EXPERTS, dtype=jnp.int32)[None, None, :]).astype(jnp.int32)
    position = jnp.sum((jnp.cumsum(onehot, axis=1) - onehot) * onehot, axis=2).astype(jnp.int32)
    entries = jnp.arange(TOKENS * 2, dtype=jnp.int32).reshape(blocks, TOK_DEV * 2)
    source = jnp.broadcast_to(jnp.arange(blocks, dtype=jnp.int32)[:, None], flat_ids.shape)
    slot_map = jnp.full((EXPERTS, blocks, CAP), -1, jnp.int32)
    slot_map = slot_map.at[flat_ids, source, position].set(entries)
    return slot_map.reshape(EXPERTS, blocks * CAP)


def reference(cotangent, layer_input, group_choice, inner_pair, group_weight, inner_logits,
              w_gate, w_up, w_down, outer_gate, inner_gate, value_stream, conv_out, conv_taps, w_out):
    slot_map = slot_table(group_choice, inner_pair)
    route = group_weight[:, None] * jax.nn.softmax(inner_logits, axis=1)
    scaled = (route[:, :, None] * cotangent.astype(jnp.float32)[:, None, :]).astype(jnp.bfloat16)
    scaled = scaled.reshape(TOKENS * 2, D)
    rows_in = jnp.repeat(layer_input, 2, axis=0)
    inner_dims = (((1,), (1,)), ((), ()))
    row_dims = (((0,), (0,)), ((), ()))
    block_width = FF // HID_BLOCKS

    def expert_pass(inputs):
        slot_index, gate_weight, up_weight, down_weight = inputs
        filled = slot_index >= 0
        clamped = jnp.maximum(slot_index, 0)
        in_rows = jnp.where(filled[:, None], rows_in[clamped], jnp.zeros((), jnp.bfloat16))
        scaled_rows = jnp.where(filled[:, None], scaled[clamped], jnp.zeros((), jnp.bfloat16))
        gate_pre = lax.dot_general(in_rows, gate_weight, inner_dims, preferred_element_type=jnp.float32)
        up_pre = lax.dot_general(in_rows, up_weight, inner_dims, preferred_element_type=jnp.float32)
        back = lax.dot_general(scaled_rows, down_weight, inner_dims, preferred_element_type=jnp.float32)
        sigmoid_gate = jax.nn.sigmoid(gate_pre)
        silu_gate = gate_pre * sigmoid_gate
        hidden = (silu_gate * up_pre).astype(jnp.bfloat16)
        grad_gate = (back * up_pre * sigmoid_gate * (1.0 + gate_pre * (1.0 - sigmoid_gate))).astype(jnp.bfloat16)
        grad_up = (back * silu_gate).astype(jnp.bfloat16)
        gate_grad = lax.dot_general(grad_gate, in_rows, row_dims, preferred_element_type=jnp.float32).astype(jnp.bfloat16)
        up_grad = lax.dot_general(grad_up, in_rows, row_dims, preferred_element_type=jnp.float32).astype(jnp.bfloat16)
        down_grad = lax.dot_general(hidden, scaled_rows, row_dims, preferred_element_type=jnp.float32).astype(jnp.bfloat16)
        blocked_gate = grad_gate.astype(jnp.float32).reshape(-1, HID_BLOCKS, block_width)
        blocked_up = grad_up.astype(jnp.float32).reshape(-1, HID_BLOCKS, block_width)
        gate_blocks = gate_weight.astype(jnp.float32).reshape(HID_BLOCKS, block_width, D)
        up_blocks = up_weight.astype(jnp.float32).reshape(HID_BLOCKS, block_width, D)
        pieces = jnp.einsum("rbf,bfd->rbd", blocked_gate, gate_blocks) + jnp.einsum("rbf,bfd->rbd", blocked_up, up_blocks)
        pieces = lax.optimization_barrier(pieces.astype(jnp.bfloat16)).astype(jnp.float32)
        returned = jnp.sum(pieces, axis=1).astype(jnp.bfloat16)
        return gate_grad, up_grad, down_grad, returned

    grad_w_gate, grad_w_up, grad_w_down, returned = lax.map(expert_pass, (slot_map, w_gate, w_up, w_down))
    targets = jnp.where(slot_map >= 0, slot_map, 2 * TOKENS).reshape(-1).astype(jnp.int32)
    collected = jnp.zeros((2 * TOKENS, D), jnp.float32).at[targets].set(
        returned.reshape(-1, D).astype(jnp.float32), mode="drop")
    collected = collected.reshape(TOKENS, 2, D)
    grad_input = (cotangent.astype(jnp.float32) + collected[:, 0] + collected[:, 1]).astype(jnp.bfloat16)

    grad_out = lax.dot_general(w_out, grad_input, (((0,), (1,)), ((), ())), preferred_element_type=jnp.float32)
    mixer_out = (outer_gate.astype(jnp.float32) * conv_out.astype(jnp.float32)).astype(jnp.bfloat16)
    grad_w_out = lax.dot_general(grad_input, mixer_out, (((0,), (1,)), ((), ())), preferred_element_type=jnp.float32)
    grad_outer_gate = (grad_out * conv_out.astype(jnp.float32)).astype(jnp.bfloat16)
    grad_conv = grad_out * outer_gate.astype(jnp.float32)
    extended = jnp.pad(grad_conv, ((0, 0), (0, TAPS - 1)))
    grad_mixed = jnp.zeros_like(grad_conv)
    for offset in range(TAPS):
        start = TAPS - 1 - offset
        grad_mixed = grad_mixed + conv_taps[offset][:, None] * extended[:, start:start + TOKENS]
    grad_inner_gate = (grad_mixed * value_stream.astype(jnp.float32)).astype(jnp.bfloat16)
    grad_value_stream = (grad_mixed * inner_gate.astype(jnp.float32)).astype(jnp.bfloat16)
    return (grad_input, grad_w_gate, grad_w_up, grad_w_down, grad_w_out,
            grad_outer_gate, grad_inner_gate, grad_value_stream)
```

```python
import functools

import jax
import jax.numpy as jnp
from jax import lax
from jax.experimental import pallas as pl
from jax.experimental.pallas import tpu as pltpu
from jax.sharding import PartitionSpec as P

TAPS = 3
INNER = 4


MESH = pl.DeviceIdType.MESH


def places(experts, rows):
    me, tp = lax.axis_index("sp"), lax.axis_index("tp")
    return me, tp // 2, lax.rem(tp, 2)


def greet(experts, rows):
    me, y, core = places(experts, rows)
    barrier = pltpu.get_barrier_semaphore()
    for step in range(1, experts):
        pl.semaphore_signal(
            barrier, inc=1, device_id={"sp": lax.rem(me + step, experts)}, device_id_type=MESH
        )
    for step in range(1, rows):
        pl.semaphore_signal(
            barrier,
            inc=1,
            device_id={"tp": lax.rem(y + step, rows) * 2 + core},
            device_id_type=MESH,
        )
    pl.semaphore_signal(barrier, inc=1, device_id={"tp": y * 2 + 1 - core}, device_id_type=MESH)
    pl.semaphore_wait(barrier, experts + rows - 1)


def dispatch_kernel(
    experts, rows, x_ref, out_ref, s_sem, r_sem, ys_sem, yr_sem, ps_sem, pr_sem
):
    me, y, core = places(experts, rows)
    width = x_ref.shape[-1]

    def block(source, row, side):
        column = pl.multiple_of((row * 2 + side) * width, width)
        return out_ref.at[:, source, :, pl.ds(column, width)]

    def across(step):
        target = lax.rem(me + step, experts)
        return pltpu.make_async_remote_copy(
            src_ref=x_ref.at[:, target],
            dst_ref=block(me, y, core),
            send_sem=s_sem.at[step],
            recv_sem=r_sem.at[step],
            device_id={"sp": target},
            device_id_type=MESH,
        )

    def to_row(hop, step, own):
        source = lax.rem(me - step + experts, experts)
        return pltpu.make_async_remote_copy(
            src_ref=x_ref.at[:, me] if own else block(source, y, core),
            dst_ref=block(source, y, core),
            send_sem=ys_sem.at[hop, step],
            recv_sem=yr_sem.at[hop, step],
            device_id={"tp": lax.rem(y + hop, rows) * 2 + core},
            device_id_type=MESH,
        )

    def to_partner(hop, step, own):
        source = lax.rem(me - step + experts, experts)
        row = lax.rem(y - hop + rows, rows)
        return pltpu.make_async_remote_copy(
            src_ref=x_ref.at[:, me] if own else block(source, row, core),
            dst_ref=block(source, row, core),
            send_sem=ps_sem.at[hop, step],
            recv_sem=pr_sem.at[hop, step],
            device_id={"tp": y * 2 + 1 - core},
            device_id_type=MESH,
        )

    def loop(start, body):
        lax.fori_loop(start, experts, lambda step, carry: (body(step), carry)[1], 0)

    greet(experts, rows)
    for hop in range(1, rows):
        to_row(hop, 0, True).start()
    loop(1, lambda step: across(step).start())
    to_partner(0, 0, True).start()
    own_column = pl.multiple_of((y * 2 + core) * width, width)
    for kind in range(x_ref.shape[0]):
        out_ref[kind, me, :, pl.ds(own_column, width)] = x_ref[kind, me]

    def forward(step):
        across(step).wait_recv()
        for hop in range(1, rows):
            to_row(hop, step, False).start()
        to_partner(0, step, False).start()
        for hop in range(1, rows):
            to_row(hop, step - 1, False).wait_recv()
            to_partner(hop, step - 1, False).start()

    loop(1, forward)
    for hop in range(1, rows):
        to_row(hop, experts - 1, False).wait_recv()
        to_partner(hop, experts - 1, False).start()

    def finish(step):
        for hop in range(rows):
            to_partner(hop, step, False).wait()
        for hop in range(1, rows):
            to_row(hop, step, False).wait_send()

    loop(0, finish)
    loop(1, lambda step: across(step).wait_send())


def dispatch(packed, experts, rows):
    kinds, _, slots, width = packed.shape
    dma = pltpu.SemaphoreType.DMA
    return pl.pallas_call(
        functools.partial(dispatch_kernel, experts, rows),
        out_shape=jax.ShapeDtypeStruct((kinds, experts, slots, 2 * rows * width), packed.dtype),
        in_specs=[pl.BlockSpec(memory_space=pltpu.VMEM)],
        out_specs=pl.BlockSpec(memory_space=pltpu.VMEM),
        scratch_shapes=[dma((experts,))] * 2 + [dma((rows, experts))] * 4,
        compiler_params=pltpu.CompilerParams(collective_id=0, has_side_effects=True),
    )(packed)


def combine_kernel(
    experts,
    rows,
    x_ref,
    out_ref,
    from_partner,
    row_out,
    row_in,
    total,
    ps_sem,
    pr_sem,
    ys_sem,
    yr_sem,
    s_sem,
    r_sem,
):
    me, y, core = places(experts, rows)
    width = out_ref.shape[-1]

    def columns(row, side):
        return pl.ds(pl.multiple_of((row * 2 + side) * width, width), width)

    def to_partner(hop):
        row = lax.rem(y + hop, rows)
        return pltpu.make_async_remote_copy(
            src_ref=x_ref.at[:, :, columns(row, 1 - core)],
            dst_ref=from_partner.at[hop],
            send_sem=ps_sem.at[hop],
            recv_sem=pr_sem.at[hop],
            device_id={"tp": y * 2 + 1 - core},
            device_id_type=MESH,
        )

    def to_row(hop, step):
        return pltpu.make_async_remote_copy(
            src_ref=row_out.at[hop, step],
            dst_ref=row_in.at[hop, step],
            send_sem=ys_sem.at[hop, step],
            recv_sem=yr_sem.at[hop, step],
            device_id={"tp": lax.rem(y + hop, rows) * 2 + core},
            device_id_type=MESH,
        )

    def across(step):
        return pltpu.make_async_remote_copy(
            src_ref=total.at[step],
            dst_ref=out_ref.at[me],
            send_sem=s_sem.at[step],
            recv_sem=r_sem.at[step],
            device_id={"sp": lax.rem(me + step, experts)},
            device_id_type=MESH,
        )

    def pair(hop, step):
        target = lax.rem(me + step, experts)
        own = x_ref[target, :, columns(lax.rem(y + hop, rows), core)].astype(jnp.float32)
        return own + from_partner[hop, target].astype(jnp.float32)

    def loop(start, body):
        lax.fori_loop(start, experts, lambda step, carry: (body(step), carry)[1], 0)

    def send_row(hop, step):
        row_out[hop, step] = pair(hop, step).astype(jnp.bfloat16)
        to_row(hop, step).start()

    def whole(step):
        value = pair(0, step)
        for hop in range(1, rows):
            to_row(hop, step).wait_recv()
            value = value + row_in[hop, step].astype(jnp.float32)
        return value.astype(jnp.bfloat16)

    def send_across(step):
        total[step] = whole(step)
        across(step).start()

    greet(experts, rows)
    for hop in [*range(1, rows), 0]:
        to_partner(hop).start()
    for hop in range(1, rows):
        to_partner(hop).wait_recv()
        loop(1, functools.partial(send_row, hop))
        send_row(hop, 0)
    to_partner(0).wait_recv()
    loop(1, send_across)
    out_ref[me] = whole(0)

    def finish(step):
        for hop in range(1, rows):
            to_row(hop, step).wait_send()

    loop(0, finish)
    loop(1, lambda step: across(step).wait())
    for hop in range(rows):
        to_partner(hop).wait_send()


def combine(partial, experts, rows):
    _, slots, full = partial.shape
    width = full // (2 * rows)
    dma = pltpu.SemaphoreType.DMA
    held = pltpu.VMEM((rows, experts, slots, width), partial.dtype)
    return pl.pallas_call(
        functools.partial(combine_kernel, experts, rows),
        out_shape=jax.ShapeDtypeStruct((experts, slots, width), partial.dtype),
        in_specs=[pl.BlockSpec(memory_space=pltpu.VMEM)],
        out_specs=pl.BlockSpec(memory_space=pltpu.VMEM),
        scratch_shapes=[held] * 3
        + [pltpu.VMEM((experts, slots, width), partial.dtype)]
        + [dma((rows,))] * 2
        + [dma((rows, experts))] * 2
        + [dma((experts,))] * 2,
        compiler_params=pltpu.CompilerParams(collective_id=1, has_side_effects=True),
    )(partial)


def from_behind(value, axis, steps):
    count = lax.axis_size(axis)
    first, last = (max(0, -steps), min(count, count - steps))
    return lax.ppermute(value, axis, [(source, source + steps) for source in range(first, last)])


def pack_rows(input_rows, cot_rows, token_of, entry_of, filled, routing_flat, experts, capacity):
    picked = jnp.where(filled[:, None], input_rows[token_of], jnp.zeros((), jnp.bfloat16))
    weighted = routing_flat[entry_of][:, None] * cot_rows[token_of].astype(jnp.float32)
    scaled = jnp.where(filled[:, None], weighted, 0.0).astype(jnp.bfloat16)
    return (picked.reshape(experts, capacity, -1), scaled.reshape(experts, capacity, -1))


def per_device(
    cotangent,
    layer_input,
    group_choice,
    inner_pair,
    group_weight,
    inner_logits,
    w_gate,
    w_up,
    w_down,
    outer_gate,
    inner_gate,
    value_stream,
    conv_out,
    conv_taps,
    w_out,
):
    experts = lax.axis_size("sp")
    tok_rows = cotangent.shape[0]
    model_width = cotangent.shape[1]
    col_piece = model_width // lax.axis_size("tp")
    column = lax.axis_index("tp") * col_piece
    group_count = experts // INNER
    capacity = 4 * (3 * tok_rows // (16 * group_count) + 1)
    capacity = -(-capacity // 8) * 8
    tp_rows = lax.axis_size("tp") // 2
    mixer_out = (outer_gate.astype(jnp.float32) * conv_out.astype(jnp.float32)).astype(jnp.bfloat16)
    mixer_all = lax.all_gather(mixer_out.T, "sp", axis=0, tiled=True)
    entry_count = 2 * tok_rows
    expert_ids = (INNER * group_choice[:, None] + inner_pair).reshape(-1)
    onehot = (expert_ids[:, None] == jnp.arange(experts, dtype=jnp.int32)[None, :]).astype(
        jnp.int32
    )
    position = jnp.sum((jnp.cumsum(onehot, axis=0) - onehot) * onehot, axis=1)
    target = expert_ids * capacity + position
    source = (
        jnp.full((experts * capacity,), entry_count, jnp.int32)
        .at[target]
        .set(jnp.arange(entry_count, dtype=jnp.int32))
    )
    filled = source < entry_count
    entry_of = jnp.minimum(source, entry_count - 1)
    token_of = entry_of // 2
    routing = group_weight[:, None] * jax.nn.softmax(inner_logits, axis=1)
    routing_flat = routing.reshape(-1)
    input_cols = lax.dynamic_slice_in_dim(layer_input, column, col_piece, 1)
    cot_cols = lax.dynamic_slice_in_dim(cotangent, column, col_piece, 1)
    input_send, scaled_send = pack_rows(
        input_cols, cot_cols, token_of, entry_of, filled, routing_flat, experts, capacity
    )
    received = dispatch(jnp.stack([input_send, scaled_send]), experts, tp_rows)
    in_rows = received[0].reshape(-1, model_width)
    scaled_rows = received[1].reshape(-1, model_width)
    gate_weight = w_gate[0]
    up_weight = w_up[0]
    down_weight = w_down[0]
    inner_dims = (((1,), (1,)), ((), ()))
    row_dims = (((0,), (0,)), ((), ()))
    gate_pre = lax.dot_general(in_rows, gate_weight, inner_dims, preferred_element_type=jnp.float32)
    up_pre = lax.dot_general(in_rows, up_weight, inner_dims, preferred_element_type=jnp.float32)
    back = lax.dot_general(scaled_rows, down_weight, inner_dims, preferred_element_type=jnp.float32)
    sigmoid_gate = jax.nn.sigmoid(gate_pre)
    silu_gate = gate_pre * sigmoid_gate
    hidden = (silu_gate * up_pre).astype(jnp.bfloat16)
    grad_gate = (back * up_pre * sigmoid_gate * (1.0 + gate_pre * (1.0 - sigmoid_gate))).astype(
        jnp.bfloat16
    )
    grad_up = (back * silu_gate).astype(jnp.bfloat16)
    partial_rows = jnp.dot(grad_gate, gate_weight, preferred_element_type=jnp.float32) + jnp.dot(
        grad_up, up_weight, preferred_element_type=jnp.float32
    )
    grad_w_gate = lax.dot_general(
        grad_gate, in_rows, row_dims, preferred_element_type=jnp.float32
    ).astype(jnp.bfloat16)
    grad_w_up = lax.dot_general(
        grad_up, in_rows, row_dims, preferred_element_type=jnp.float32
    ).astype(jnp.bfloat16)
    grad_w_down = lax.dot_general(
        hidden, scaled_rows, row_dims, preferred_element_type=jnp.float32
    ).astype(jnp.bfloat16)
    returned = combine(
        partial_rows.astype(jnp.bfloat16).reshape(experts, capacity, model_width), experts, tp_rows
    )
    back_tok = (
        returned.reshape(-1, col_piece)[target].reshape(tok_rows, 2, col_piece).astype(jnp.float32)
    )
    cot_cols = lax.dynamic_slice_in_dim(cotangent, column, col_piece, 1).astype(jnp.float32)
    own_cols = (cot_cols + back_tok[:, 0] + back_tok[:, 1]).astype(jnp.bfloat16)
    grad_rows = lax.all_gather(own_cols, "tp", axis=1, tiled=True)
    grad_out = lax.dot_general(
        w_out, grad_rows, (((0,), (1,)), ((), ())), preferred_element_type=jnp.float32
    )
    grad_all = lax.all_to_all(grad_rows, "sp", split_axis=1, concat_axis=0, tiled=True)
    grad_w_out = lax.dot_general(grad_all, mixer_all, row_dims, preferred_element_type=jnp.float32)
    grad_outer_gate = (grad_out * conv_out.astype(jnp.float32)).astype(jnp.bfloat16)
    grad_conv = grad_out * outer_gate.astype(jnp.float32)
    following = from_behind(grad_conv[:, : TAPS - 1], "sp", -1)
    extended = jnp.concatenate([grad_conv, following], axis=1)
    grad_mixed = jnp.zeros_like(grad_conv)
    for offset in range(TAPS):
        start = TAPS - 1 - offset
        grad_mixed = grad_mixed + conv_taps[offset][:, None] * extended[:, start : start + tok_rows]
    grad_inner_gate = (grad_mixed * value_stream.astype(jnp.float32)).astype(jnp.bfloat16)
    grad_value_stream = (grad_mixed * inner_gate.astype(jnp.float32)).astype(jnp.bfloat16)
    return (
        own_cols,
        grad_w_gate[None],
        grad_w_up[None],
        grad_w_down[None],
        grad_w_out,
        grad_outer_gate,
        grad_inner_gate,
        grad_value_stream,
    )


def solution(mesh):
    return jax.shard_map(
        per_device,
        mesh=mesh,
        in_specs=(
            P("sp", None),
            P("sp", None),
            P("sp"),
            P("sp", None),
            P("sp"),
            P("sp", None),
            P("sp", "tp", None),
            P("sp", "tp", None),
            P("sp", "tp", None),
            P("tp", "sp"),
            P("tp", "sp"),
            P("tp", "sp"),
            P("tp", "sp"),
            P(None, "tp"),
            P(None, "tp"),
        ),
        out_specs=(
            P("sp", "tp"),
            P("sp", "tp", None),
            P("sp", "tp", None),
            P("sp", "tp", None),
            P("sp", "tp"),
            P("tp", "sp"),
            P("tp", "sp"),
            P("tp", "sp"),
        ),
        check_vma=False,
    )
```

```python
import functools

import jax
import jax.numpy as jnp
from jax import lax
from jax.experimental import pallas as pl
from jax.experimental.pallas import tpu as pltpu
from jax.sharding import PartitionSpec as P

TAPS = 3
INNER = 4


MESH = pl.DeviceIdType.MESH


def places(experts, rows):
    me, tp = lax.axis_index("sp"), lax.axis_index("tp")
    return me, tp // 2, lax.rem(tp, 2)


def greet(experts, rows):
    me, y, core = places(experts, rows)
    barrier = pltpu.get_barrier_semaphore()
    for step in range(1, experts):
        pl.semaphore_signal(
            barrier, inc=1, device_id={"sp": lax.rem(me + step, experts)}, device_id_type=MESH
        )
    for step in range(1, rows):
        pl.semaphore_signal(
            barrier,
            inc=1,
            device_id={"tp": lax.rem(y + step, rows) * 2 + core},
            device_id_type=MESH,
        )
    pl.semaphore_signal(barrier, inc=1, device_id={"tp": y * 2 + 1 - core}, device_id_type=MESH)
    pl.semaphore_wait(barrier, experts + rows - 1)


def dispatch_kernel(
    experts, rows, x_ref, out_ref, s_sem, r_sem, ys_sem, yr_sem, ps_sem, pr_sem
):
    me, y, core = places(experts, rows)
    width = x_ref.shape[-1]

    def block(source, row, side):
        column = pl.multiple_of((row * 2 + side) * width, width)
        return out_ref.at[:, source, :, pl.ds(column, width)]

    def across(step):
        target = lax.rem(me + step, experts)
        return pltpu.make_async_remote_copy(
            src_ref=x_ref.at[:, target],
            dst_ref=block(me, y, core),
            send_sem=s_sem.at[step],
            recv_sem=r_sem.at[step],
            device_id={"sp": target},
            device_id_type=MESH,
        )

    def to_row(hop, step, own):
        source = lax.rem(me - step + experts, experts)
        return pltpu.make_async_remote_copy(
            src_ref=x_ref.at[:, me] if own else block(source, y, core),
            dst_ref=block(source, y, core),
            send_sem=ys_sem.at[hop, step],
            recv_sem=yr_sem.at[hop, step],
            device_id={"tp": lax.rem(y + hop, rows) * 2 + core},
            device_id_type=MESH,
        )

    def to_partner(hop, step, own):
        source = lax.rem(me - step + experts, experts)
        row = lax.rem(y - hop + rows, rows)
        return pltpu.make_async_remote_copy(
            src_ref=x_ref.at[:, me] if own else block(source, row, core),
            dst_ref=block(source, row, core),
            send_sem=ps_sem.at[hop, step],
            recv_sem=pr_sem.at[hop, step],
            device_id={"tp": y * 2 + 1 - core},
            device_id_type=MESH,
        )

    def loop(start, body):
        lax.fori_loop(start, experts, lambda step, carry: (body(step), carry)[1], 0)

    greet(experts, rows)
    for hop in range(1, rows):
        to_row(hop, 0, True).start()
    loop(1, lambda step: across(step).start())
    to_partner(0, 0, True).start()
    own_column = pl.multiple_of((y * 2 + core) * width, width)
    for kind in range(x_ref.shape[0]):
        out_ref[kind, me, :, pl.ds(own_column, width)] = x_ref[kind, me]

    def forward(step):
        across(step).wait_recv()
        for hop in range(1, rows):
            to_row(hop, step, False).start()
        to_partner(0, step, False).start()
        for hop in range(1, rows):
            to_row(hop, step - 1, False).wait_recv()
            to_partner(hop, step - 1, False).start()

    loop(1, forward)
    for hop in range(1, rows):
        to_row(hop, experts - 1, False).wait_recv()
        to_partner(hop, experts - 1, False).start()

    def finish(step):
        for hop in range(rows):
            to_partner(hop, step, False).wait()
        for hop in range(1, rows):
            to_row(hop, step, False).wait_send()

    loop(0, finish)
    loop(1, lambda step: across(step).wait_send())


def dispatch(packed, experts, rows):
    kinds, _, slots, width = packed.shape
    dma = pltpu.SemaphoreType.DMA
    return pl.pallas_call(
        functools.partial(dispatch_kernel, experts, rows),
        out_shape=jax.ShapeDtypeStruct((kinds, experts, slots, 2 * rows * width), packed.dtype),
        in_specs=[pl.BlockSpec(memory_space=pltpu.VMEM)],
        out_specs=pl.BlockSpec(memory_space=pltpu.VMEM),
        scratch_shapes=[dma((experts,))] * 2 + [dma((rows, experts))] * 4,
        compiler_params=pltpu.CompilerParams(collective_id=0, has_side_effects=True),
    )(packed)


def combine_kernel(
    experts,
    rows,
    x_ref,
    mixer_ref,
    out_ref,
    mixer_all,
    from_partner,
    row_out,
    row_in,
    total,
    ps_sem,
    pr_sem,
    ys_sem,
    yr_sem,
    s_sem,
    r_sem,
    ms_sem,
    mr_sem,
    ns_sem,
    nr_sem,
):
    me, y, core = places(experts, rows)
    halves = experts // 2
    half, side_of = me // 2, lax.rem(me, 2)
    width = out_ref.shape[-1]

    def columns(row, side):
        return pl.ds(pl.multiple_of((row * 2 + side) * width, width), width)

    def to_partner(hop):
        row = lax.rem(y + hop, rows)
        return pltpu.make_async_remote_copy(
            src_ref=x_ref.at[:, :, columns(row, 1 - core)],
            dst_ref=from_partner.at[hop],
            send_sem=ps_sem.at[hop],
            recv_sem=pr_sem.at[hop],
            device_id={"tp": y * 2 + 1 - core},
            device_id_type=MESH,
        )

    def to_row(hop, step):
        return pltpu.make_async_remote_copy(
            src_ref=row_out.at[hop, step],
            dst_ref=row_in.at[hop, step],
            send_sem=ys_sem.at[hop, step],
            recv_sem=yr_sem.at[hop, step],
            device_id={"tp": lax.rem(y + hop, rows) * 2 + core},
            device_id_type=MESH,
        )

    def across(step):
        return pltpu.make_async_remote_copy(
            src_ref=total.at[step],
            dst_ref=out_ref.at[me],
            send_sem=s_sem.at[step],
            recv_sem=r_sem.at[step],
            device_id={"sp": lax.rem(me + step, experts)},
            device_id_type=MESH,
        )

    def mixer_along(hop):
        return pltpu.make_async_remote_copy(
            src_ref=mixer_ref,
            dst_ref=mixer_all.at[me],
            send_sem=ms_sem.at[hop],
            recv_sem=mr_sem.at[hop],
            device_id={"sp": lax.rem(half + hop, halves) * 2 + side_of},
            device_id_type=MESH,
        )

    def mixer_beside(hop, own):
        source = lax.rem(half - hop + halves, halves) * 2 + side_of
        return pltpu.make_async_remote_copy(
            src_ref=mixer_ref if own else mixer_all.at[source],
            dst_ref=mixer_all.at[source],
            send_sem=ns_sem.at[hop],
            recv_sem=nr_sem.at[hop],
            device_id={"sp": half * 2 + 1 - side_of},
            device_id_type=MESH,
        )

    def pair(hop, step):
        target = lax.rem(me + step, experts)
        own = x_ref[target, :, columns(lax.rem(y + hop, rows), core)].astype(jnp.float32)
        return own + from_partner[hop, target].astype(jnp.float32)

    def loop(start, body):
        lax.fori_loop(start, experts, lambda step, carry: (body(step), carry)[1], 0)

    def send_row(hop, step):
        row_out[hop, step] = pair(hop, step).astype(jnp.bfloat16)
        to_row(hop, step).start()

    def whole(step):
        value = pair(0, step)
        for hop in range(1, rows):
            to_row(hop, step).wait_recv()
            value = value + row_in[hop, step].astype(jnp.float32)
        return value.astype(jnp.bfloat16)

    def send_across(step):
        total[step] = whole(step)
        across(step).start()

    greet(experts, rows)
    for hop in [*range(1, rows), 0]:
        to_partner(hop).start()
    for hop in range(1, halves):
        mixer_along(hop).start()
    mixer_beside(0, True).start()
    mixer_all[me] = mixer_ref[...]
    for hop in range(1, rows):
        to_partner(hop).wait_recv()
        loop(1, functools.partial(send_row, hop))
        send_row(hop, 0)
    to_partner(0).wait_recv()
    loop(1, send_across)
    out_ref[me] = whole(0)
    for hop in range(1, halves):
        mixer_along(hop).wait_recv()
        mixer_beside(hop, False).start()

    def finish(step):
        for hop in range(1, rows):
            to_row(hop, step).wait_send()

    loop(0, finish)
    loop(1, lambda step: across(step).wait())
    for hop in range(rows):
        to_partner(hop).wait_send()
    for hop in range(halves):
        mixer_beside(hop, False).wait()
    for hop in range(1, halves):
        mixer_along(hop).wait_send()


def combine(partial, mixer, experts, rows):
    _, slots, full = partial.shape
    width = full // (2 * rows)
    dma = pltpu.SemaphoreType.DMA
    held = pltpu.VMEM((rows, experts, slots, width), partial.dtype)
    return pl.pallas_call(
        functools.partial(combine_kernel, experts, rows),
        out_shape=(
            jax.ShapeDtypeStruct((experts, slots, width), partial.dtype),
            jax.ShapeDtypeStruct((experts, *mixer.shape), mixer.dtype),
        ),
        in_specs=[pl.BlockSpec(memory_space=pltpu.VMEM)] * 2,
        out_specs=(pl.BlockSpec(memory_space=pltpu.VMEM),) * 2,
        scratch_shapes=[held] * 3
        + [pltpu.VMEM((experts, slots, width), partial.dtype)]
        + [dma((rows,))] * 2
        + [dma((rows, experts))] * 2
        + [dma((experts,))] * 2
        + [dma((experts // 2,))] * 4,
        compiler_params=pltpu.CompilerParams(collective_id=1, has_side_effects=True),
    )(partial, mixer)


def from_behind(value, axis, steps):
    count = lax.axis_size(axis)
    first, last = (max(0, -steps), min(count, count - steps))
    return lax.ppermute(value, axis, [(source, source + steps) for source in range(first, last)])


def pack_rows(input_rows, cot_rows, token_of, entry_of, filled, routing_flat, experts, capacity):
    picked = jnp.where(filled[:, None], input_rows[token_of], jnp.zeros((), jnp.bfloat16))
    weighted = routing_flat[entry_of][:, None] * cot_rows[token_of].astype(jnp.float32)
    scaled = jnp.where(filled[:, None], weighted, 0.0).astype(jnp.bfloat16)
    return (picked.reshape(experts, capacity, -1), scaled.reshape(experts, capacity, -1))


def per_device(
    cotangent,
    layer_input,
    group_choice,
    inner_pair,
    group_weight,
    inner_logits,
    w_gate,
    w_up,
    w_down,
    outer_gate,
    inner_gate,
    value_stream,
    conv_out,
    conv_taps,
    w_out,
):
    experts = lax.axis_size("sp")
    tok_rows = cotangent.shape[0]
    model_width = cotangent.shape[1]
    col_piece = model_width // lax.axis_size("tp")
    column = lax.axis_index("tp") * col_piece
    group_count = experts // INNER
    capacity = 4 * (3 * tok_rows // (16 * group_count) + 1)
    capacity = -(-capacity // 8) * 8
    tp_rows = lax.axis_size("tp") // 2
    mixer_out = (outer_gate.astype(jnp.float32) * conv_out.astype(jnp.float32)).astype(jnp.bfloat16)
    entry_count = 2 * tok_rows
    expert_ids = (INNER * group_choice[:, None] + inner_pair).reshape(-1)
    onehot = (expert_ids[:, None] == jnp.arange(experts, dtype=jnp.int32)[None, :]).astype(
        jnp.int32
    )
    position = jnp.sum((jnp.cumsum(onehot, axis=0) - onehot) * onehot, axis=1)
    target = expert_ids * capacity + position
    source = (
        jnp.full((experts * capacity,), entry_count, jnp.int32)
        .at[target]
        .set(jnp.arange(entry_count, dtype=jnp.int32))
    )
    filled = source < entry_count
    entry_of = jnp.minimum(source, entry_count - 1)
    token_of = entry_of // 2
    routing = group_weight[:, None] * jax.nn.softmax(inner_logits, axis=1)
    routing_flat = routing.reshape(-1)
    input_cols = lax.dynamic_slice_in_dim(layer_input, column, col_piece, 1)
    cot_cols = lax.dynamic_slice_in_dim(cotangent, column, col_piece, 1)
    input_send, scaled_send = pack_rows(
        input_cols, cot_cols, token_of, entry_of, filled, routing_flat, experts, capacity
    )
    received = dispatch(jnp.stack([input_send, scaled_send]), experts, tp_rows)
    in_rows = received[0].reshape(-1, model_width)
    scaled_rows = received[1].reshape(-1, model_width)
    gate_weight = w_gate[0]
    up_weight = w_up[0]
    down_weight = w_down[0]
    inner_dims = (((1,), (1,)), ((), ()))
    row_dims = (((0,), (0,)), ((), ()))
    gate_pre = lax.dot_general(in_rows, gate_weight, inner_dims, preferred_element_type=jnp.float32)
    up_pre = lax.dot_general(in_rows, up_weight, inner_dims, preferred_element_type=jnp.float32)
    back = lax.dot_general(scaled_rows, down_weight, inner_dims, preferred_element_type=jnp.float32)
    sigmoid_gate = jax.nn.sigmoid(gate_pre)
    silu_gate = gate_pre * sigmoid_gate
    hidden = (silu_gate * up_pre).astype(jnp.bfloat16)
    grad_gate = (back * up_pre * sigmoid_gate * (1.0 + gate_pre * (1.0 - sigmoid_gate))).astype(
        jnp.bfloat16
    )
    grad_up = (back * silu_gate).astype(jnp.bfloat16)
    partial_rows = jnp.dot(grad_gate, gate_weight, preferred_element_type=jnp.float32) + jnp.dot(
        grad_up, up_weight, preferred_element_type=jnp.float32
    )
    grad_w_gate = lax.dot_general(
        grad_gate, in_rows, row_dims, preferred_element_type=jnp.float32
    ).astype(jnp.bfloat16)
    grad_w_up = lax.dot_general(
        grad_up, in_rows, row_dims, preferred_element_type=jnp.float32
    ).astype(jnp.bfloat16)
    grad_w_down = lax.dot_general(
        hidden, scaled_rows, row_dims, preferred_element_type=jnp.float32
    ).astype(jnp.bfloat16)
    returned, mixer_all = combine(
        partial_rows.astype(jnp.bfloat16).reshape(experts, capacity, model_width),
        mixer_out.T,
        experts,
        tp_rows,
    )
    mixer_all = mixer_all.reshape(-1, mixer_all.shape[-1])
    back_tok = (
        returned.reshape(-1, col_piece)[target].reshape(tok_rows, 2, col_piece).astype(jnp.float32)
    )
    cot_cols = lax.dynamic_slice_in_dim(cotangent, column, col_piece, 1).astype(jnp.float32)
    own_cols = (cot_cols + back_tok[:, 0] + back_tok[:, 1]).astype(jnp.bfloat16)
    grad_rows = lax.all_gather(own_cols, "tp", axis=1, tiled=True)
    grad_out = lax.dot_general(
        w_out, grad_rows, (((0,), (1,)), ((), ())), preferred_element_type=jnp.float32
    )
    grad_all = lax.all_to_all(grad_rows, "sp", split_axis=1, concat_axis=0, tiled=True)
    grad_w_out = lax.dot_general(grad_all, mixer_all, row_dims, preferred_element_type=jnp.float32)
    grad_outer_gate = (grad_out * conv_out.astype(jnp.float32)).astype(jnp.bfloat16)
    grad_conv = grad_out * outer_gate.astype(jnp.float32)
    following = from_behind(grad_conv[:, : TAPS - 1], "sp", -1)
    extended = jnp.concatenate([grad_conv, following], axis=1)
    grad_mixed = jnp.zeros_like(grad_conv)
    for offset in range(TAPS):
        start = TAPS - 1 - offset
        grad_mixed = grad_mixed + conv_taps[offset][:, None] * extended[:, start : start + tok_rows]
    grad_inner_gate = (grad_mixed * value_stream.astype(jnp.float32)).astype(jnp.bfloat16)
    grad_value_stream = (grad_mixed * inner_gate.astype(jnp.float32)).astype(jnp.bfloat16)
    return (
        own_cols,
        grad_w_gate[None],
        grad_w_up[None],
        grad_w_down[None],
        grad_w_out,
        grad_outer_gate,
        grad_inner_gate,
        grad_value_stream,
    )


def solution(mesh):
    return jax.shard_map(
        per_device,
        mesh=mesh,
        in_specs=(
            P("sp", None),
            P("sp", None),
            P("sp"),
            P("sp", None),
            P("sp"),
            P("sp", None),
            P("sp", "tp", None),
            P("sp", "tp", None),
            P("sp", "tp", None),
            P("tp", "sp"),
            P("tp", "sp"),
            P("tp", "sp"),
            P("tp", "sp"),
            P(None, "tp"),
            P(None, "tp"),
        ),
        out_specs=(
            P("sp", "tp"),
            P("sp", "tp", None),
            P("sp", "tp", None),
            P("sp", "tp", None),
            P("sp", "tp"),
            P("tp", "sp"),
            P("tp", "sp"),
            P("tp", "sp"),
        ),
        check_vma=False,
    )
```
